32 devices in a mesh: fs: 16 (over z, y, x), tp: 2 (over core).
Axes of the slice: x: 2, y: 2, z: 4, core: 2. Of those that a mesh axis runs over, the one named last changes fastest.
Arguments:
- normed_input: bfloat16 [8192, 2048], P('fs', 'tp'), may hold values from -6 to 6
- cotangent: bfloat16 [8192, 2048], P('fs', 'tp'), may hold values from -6 to 6
- up_weight: bfloat16 [2048, 8192], P('fs', 'tp'), may hold values from -0.125 to 0.125
- down_weight: bfloat16 [8192, 2048], P('tp', 'fs'), may hold values from -0.0625 to 0.0625
Outputs:
- input_grad: bfloat16 [8192, 2048], P('fs', 'tp')
- up_grad: float32 [2048, 8192], P('fs', 'tp')
- down_grad: float32 [8192, 2048], P('tp', 'fs')
The draws below stay inside these ranges and needn't reach their ends.
All inputs are finite; a program needn't handle non-finite values.
Results may differ from the reference program's by a relative error of at most 0.018.
Values may be sent and summed in bfloat16 or wider, within the bound.
A program may use at most 192 MiB of HBM per device.

```python
import jax
import jax.numpy as jnp
from jax import lax

D = 2048
FF = 8192
TOKENS = 8192
FF_BLOCKS = 2


def strengthened(array, key, source, target, blocks, factor):
    owner, partner = [(jnp.arange(array.shape[axis_at]) // (array.shape[axis_at] // blocks)).reshape([-1 if axis == axis_at else 1 for axis in range(array.ndim)]) for axis_at in (source, target)]
    chosen = jax.random.permutation(key, blocks)[partner]
    strong = (owner == chosen) | (owner == (partner + blocks // 2) % blocks)
    return jnp.where(strong, factor * array, array)


def steps_of(stream_key, extent, shards, smallest, top_value):
    gain = 1.0
    for position, shards_of in shards:
        steps = jax.random.uniform(jax.random.fold_in(jax.random.fold_in(stream_key, 6), position), (shards_of,), jnp.float32, smallest / len(shards), top_value / len(shards))
        gain = gain * jnp.repeat(jnp.exp(steps), extent[position] // shards_of).reshape((-1,) + (1,) * (len(extent) - 1 - position))
    return gain


def bell_draw(stream_key, dims, spread, limit, pieces=(), kind=jnp.bfloat16):
    array = spread * jax.random.normal(stream_key, dims, jnp.float32)
    if pieces:
        array = array * steps_of(stream_key, dims, pieces, -0.22, 0.18)
    return jnp.clip(array, -limit, limit).astype(kind)


def heavy_noise(own_key, extent, spread, limit, cuts, heavy, kind=jnp.bfloat16):
    result = spread * jax.random.normal(own_key, extent, jnp.float32)
    if cuts:
        result = result * steps_of(own_key, extent, cuts, -0.22, 0.18)
    return jnp.clip(strengthened(result, jax.random.fold_in(own_key, 3), *heavy), -limit, limit).astype(kind)


def setup_inputs(seed: int = 0) -> dict:
    splits = jax.random.split(jax.random.key(seed), 5)
    normed_input = heavy_noise(splits[0], (TOKENS, D), 1.0, 6.0, ((0, 16), (1, 2)), (0, 1, 16, 2.0))
    cotangent = heavy_noise(splits[1], (TOKENS, D), 1.0, 6.0, ((0, 16), (1, 2)), (0, 1, 16, 2.0))
    up_weight = bell_draw(splits[2], (D, FF), D ** -0.5, 0.125, ((0, 16), (1, 2)))
    down_weight = bell_draw(splits[3], (FF, D), FF ** -0.5, 0.0625, ((0, 2), (1, 16)))
    return {"normed_input": normed_input, "cotangent": cotangent, "up_weight": up_weight, "down_weight": down_weight}


def reference(normed_input, cotangent, up_weight, down_weight):
    tokens = normed_input.shape[0]
    width = FF // FF_BLOCKS
    scale = lax.rsqrt(jnp.asarray(tokens, jnp.float32))

    def block(total, index):
        start = (index * width).astype(jnp.int32)
        up_block = lax.dynamic_slice_in_dim(up_weight, start, width, 1)
        down_block = lax.dynamic_slice_in_dim(down_weight, start, width, 0)
        pre = jnp.dot(normed_input, up_block, preferred_element_type=jnp.float32)
        rectified = jax.nn.relu(pre)
        act = (rectified * rectified).astype(jnp.bfloat16)
        act_grad = jnp.dot(cotangent, down_block.T, preferred_element_type=jnp.float32)
        pre_grad = (2.0 * rectified * act_grad).astype(jnp.bfloat16)
        down_part = jnp.dot(act.T, cotangent, preferred_element_type=jnp.float32) * scale
        up_part = jnp.dot(normed_input.T, pre_grad, preferred_element_type=jnp.float32) * scale
        partial_value = jnp.dot(pre_grad, up_block.T, preferred_element_type=jnp.float32).astype(jnp.bfloat16)
        partial_value = lax.optimization_barrier(partial_value)
        return (total + partial_value.astype(jnp.float32), (up_part, down_part))
    start_total = jnp.zeros(normed_input.shape, jnp.float32)
    total, parts = lax.scan(block, start_total, jnp.arange(FF_BLOCKS, dtype=jnp.int32))
    up_parts, down_parts = parts
    up_grad = jnp.moveaxis(up_parts, 0, 1).reshape(D, FF)
    down_grad = down_parts.reshape(FF, D)
    return (total.astype(jnp.bfloat16), up_grad, down_grad)
```

```python
import functools

import jax
import jax.numpy as jnp
from jax import lax
from jax.experimental import pallas as pl
from jax.experimental.pallas import tpu as pltpu
from jax.sharding import Mesh, PartitionSpec as P


def hidden_ways(size):
    return 4 if size % 4 == 0 and size > 4 else 1


def right_product(left, right):
    return lax.dot_general(
        left, right, (((1,), (1,)), ((), ())), preferred_element_type=jnp.float32
    )


def left_product(left, right):
    return lax.dot_general(
        left, right, (((0,), (0,)), ((), ())), preferred_element_type=jnp.float32
    )


def swap(array, k):
    ways = lax.axis_size("hid")
    return lax.ppermute(array, "hid", [(i, i ^ k) for i in range(ways)])


def gather_tokens(array):
    ways = lax.axis_size("hid")
    pieces = [array] + [swap(array, k) for k in range(1, ways)]
    array = jnp.concatenate(pieces, axis=0)
    return lax.all_gather(array, "tp", axis=1, tiled=True)


def scatter_tokens(array):
    ways = lax.axis_size("hid")
    pieces = jnp.split(array, ways, axis=0)
    total = pieces[0].astype(jnp.float32)
    for k in range(1, ways):
        total = total + swap(pieces[k], k).astype(jnp.float32)
    return total.astype(array.dtype)


def exchange(blocks):
    ways, me = lax.axis_size("hid"), lax.axis_index("hid")
    got = []
    for k in range(ways):
        block = lax.dynamic_index_in_dim(blocks, me ^ k, 0, keepdims=False)
        got.append(swap(block, k) if k else block)
    got = jnp.stack(got)
    return [
        lax.dynamic_index_in_dim(got, me ^ j, 0, keepdims=False) for j in range(ways)
    ]


def weight_columns(shard):
    ways = lax.axis_size("hid")
    depth, width = shard.shape
    blocks = jnp.moveaxis(shard.reshape(depth, ways, width // ways), 1, 0)
    return jnp.concatenate(exchange(blocks), axis=0)


def scatter_grad(term):
    ways = lax.axis_size("hid")
    width = term.shape[1]
    term = lax.psum_scatter(term, "tok", scatter_dimension=0, tiled=True)
    return jnp.concatenate(exchange(term.reshape(ways, -1, width)), axis=1)


def per_device(normed_input, cotangent, up_weight, down_weight):
    tokens = normed_input.shape[0] * lax.axis_size("tok") * lax.axis_size("hid")
    scale = lax.rsqrt(jnp.asarray(tokens, jnp.float32))
    up_rows = weight_columns(up_weight)
    down_rows = weight_columns(down_weight.T)
    up_rows, down_rows, normed_input, cotangent = lax.optimization_barrier(
        (up_rows, down_rows, normed_input, cotangent)
    )
    block_up = lax.all_gather(up_rows, "tok", axis=0, tiled=True)
    block_down = lax.all_gather(down_rows, "tok", axis=0, tiled=True)
    whole_input = gather_tokens(normed_input)
    whole_cot = gather_tokens(cotangent)
    pre = jnp.dot(whole_input, block_up, preferred_element_type=jnp.float32)
    rectified = jax.nn.relu(pre)
    act = (rectified * rectified).astype(jnp.bfloat16)
    down_term = left_product(whole_cot, act) * scale
    down_grad = scatter_grad(down_term.astype(jnp.bfloat16)).astype(jnp.float32).T
    act_grad = jnp.dot(whole_cot, block_down, preferred_element_type=jnp.float32)
    pre_grad = (2.0 * rectified * act_grad).astype(jnp.bfloat16)
    up_term = left_product(whole_input, pre_grad) * scale
    up_grad = scatter_grad(up_term.astype(jnp.bfloat16)).astype(jnp.float32)
    partial_value = right_product(pre_grad, block_up).astype(jnp.bfloat16)
    input_grad = lax.psum_scatter(
        partial_value, "tp", scatter_dimension=1, tiled=True
    )
    input_grad = scatter_tokens(input_grad)
    return (input_grad, up_grad, down_grad)


def collective_solution(mesh):
    fs, tp = mesh.shape["fs"], mesh.shape["tp"]
    ways = hidden_ways(fs)
    fine = Mesh(
        mesh.devices.reshape(fs // ways, ways, tp), ("tok", "hid", "tp")
    )
    rows = ("tok", "hid")
    in_specs = (P(rows, "tp"), P(rows, "tp"), P(rows, "tp"), P("tp", rows))
    out_specs = (P(rows, "tp"), P(rows, "tp"), P("tp", rows))
    return jax.shard_map(
        per_device, mesh=fine, in_specs=in_specs, out_specs=out_specs, check_vma=False
    )


MESH = pl.DeviceIdType.MESH
CHUNKS = 4
PIECES = 2


class Links:
    def __init__(self, send, recv, local):
        self.send, self.recv, self.local = send, recv, local
        self.used, self.used_local, self.started = 0, 0, []

    def remote(self, src, dst, device):
        i = self.used
        self.used += 1
        copy = pltpu.make_async_remote_copy(
            src_ref=src,
            dst_ref=dst,
            send_sem=self.send.at[i],
            recv_sem=self.recv.at[i],
            device_id=device,
            device_id_type=MESH,
        )
        return copy

    def start(self, copy):
        copy.start()
        self.started.append(copy)

    def copy(self, src, dst):
        i = self.used_local
        self.used_local += 1
        copy = pltpu.make_async_copy(src, dst, self.local.at[i])
        copy.start()
        return copy


def loop(n, body):
    def step(i, carry):
        body(i)
        return carry

    lax.fori_loop(0, n, step, 0)


def product(left, right, left_dim, right_dim):
    return lax.dot_general(
        left,
        right,
        (((left_dim,), (right_dim,)), ((), ())),
        preferred_element_type=jnp.float32,
    )


def pair_kernel(
    scale,
    x_hbm,
    c_hbm,
    u_hbm,
    v_hbm,
    og,
    ug,
    dg,
    xs,
    cs,
    us,
    vs,
    act,
    pre_grad,
    pu,
    pv,
    rxu,
    rxv,
    rhu,
    rhv,
    own,
    sib_out,
    sib_in,
    ry,
    rl,
    send,
    recv,
    local,
    credit,
):
    bf16, f32 = jnp.bfloat16, jnp.float32
    tl, wl = x_hbm.shape
    nc, _, nq, _, rows, fc = us.shape
    fs, tp = lax.axis_index("fs"), lax.axis_index("tp")
    x, y = fs % 2, (fs // 2) % 2
    l, h = (fs // 4) % 2, fs // 8
    q, qy, ql, qd = l * 2 + y, l * 2 + 1 - y, (1 - l) * 2 + y, (1 - l) * 2 + 1 - y
    dev_x, dev_y = (fs + 1 - 2 * x, tp), (fs + 2 - 4 * y, tp)
    dev_l, dev_h = (fs + 4 - 8 * l, tp), (fs + 8 - 16 * h, tp)
    dev_d, dev_s = (fs + 6 - 4 * y - 8 * l, tp), (fs, 1 - tp)
    hid = ((dev_d, qd), (dev_y, qy), (dev_l, ql))
    links = Links(send, recv, local)
    weights = ((us, u_hbm, 1), (vs, v_hbm, 0))

    barrier = pltpu.get_barrier_semaphore()
    for device in (dev_x, dev_y, dev_l, dev_h, dev_d, dev_s):
        pl.semaphore_signal(barrier, inc=1, device_id=device, device_id_type=MESH)
    pl.semaphore_wait(barrier, 6)

    def columns(hbm, dim, block):
        span = pl.ds(pl.multiple_of(block * fc, fc), fc)
        return hbm.at[:, span] if dim else hbm.at[span, :]

    spread, mine = {}, {}
    for j in range(nc):
        for w, (buf, hbm, dim) in enumerate(weights):
            mine[w, j] = links.copy(columns(hbm, dim, q * nc + j), buf.at[j, h, q, x])
            for k, (device, other) in enumerate(hid):
                c = links.remote(
                    columns(hbm, dim, other * nc + j), buf.at[j, h, q, x], device
                )
                links.start(c)
                spread[w, j, k] = c

    tr = tl // PIECES
    mine_cols = pl.ds(pl.multiple_of(tp * wl, wl), wl)
    tokens = ((xs, x_hbm), (cs, c_hbm))

    def spot(buf, group, p):
        return buf.at[pl.ds(pl.multiple_of(group * tl + p * tr, tr), tr), mine_cols]

    own_tok, tok_l, tok_y, tok_s = {}, {}, {}, {}
    for p in range(PIECES):
        for a, (buf, hbm) in enumerate(tokens):
            src, dst = hbm.at[pl.ds(p * tr, tr), :], spot(buf, q, p)
            own_tok[a, p] = links.copy(src, dst)
            for table, device in ((tok_l, dev_l), (tok_y, dev_y), (tok_s, dev_s)):
                c = links.remote(src, dst, device)
                links.start(c)
                table[a, p, 0] = c

    far, near, second = {}, {}, {}
    for j in range(nc):
        for w, (buf, _, _) in enumerate(weights):
            mine[w, j].wait()
            for k in range(3):
                spread[w, j, k].wait_recv()
            block = buf.at[j, h, :, x]
            far[w, j] = links.remote(block, block, dev_h)
            links.start(far[w, j])
            near[w, j] = links.remote(block, block, dev_x)
            links.start(near[w, j])

    for p in range(PIECES):
        for a, (buf, _) in enumerate(tokens):
            tok_l[a, p, 0].wait_recv()
            block = spot(buf, ql, p)
            tok_y[a, p, 1] = links.remote(block, block, dev_y)
            links.start(tok_y[a, p, 1])
            tok_s[a, p, 1] = links.remote(block, block, dev_s)
            links.start(tok_s[a, p, 1])
            tok_y[a, p, 0].wait_recv()
            block = spot(buf, qy, p)
            tok_s[a, p, 2] = links.remote(block, block, dev_s)
            links.start(tok_s[a, p, 2])

    def hidden(j, groups):
        up = lambda: us[j].reshape(-1, fc)
        down = lambda: jnp.concatenate(
            [vs[j, a, b, c] for a in range(2) for b in range(nq) for c in range(2)],
            axis=1,
        )

        def one(group):
            span = pl.ds(pl.multiple_of(group * tl, tl), tl)
            pre = product(xs[span, :], up(), 1, 0)
            rectified = jnp.maximum(pre, 0.0)
            act[j, span, :] = (rectified * rectified).astype(bf16)
            act_grad = product(cs[span, :], down(), 1, 1)
            pre_grad[j, span, :] = (2.0 * rectified * act_grad).astype(bf16)

        if groups == 1:
            one(qd)
        else:
            loop(groups, lambda i: one((qd + 1 + i) % 4))

    def forward_last(i):
        p, a = i // 2, i % 2
        tok_y[a, p, 1].wait_recv()
        block = spot(tokens[a][0], qd, p)
        tok_s[a, p, 3] = links.remote(block, block, dev_s)
        links.start(tok_s[a, p, 3])

    def ready(j):
        for w in range(2):
            near[w, j].wait_recv()
            second[w, j].wait_recv()

    for j in range(nc):
        for w, (buf, _, _) in enumerate(weights):
            far[w, j].wait_recv()
            block = buf.at[j, 1 - h, :, x]
            second[w, j] = links.remote(block, block, dev_x)
            links.start(second[w, j])
        if j == 0:
            for p in range(PIECES):
                for a in range(2):
                    own_tok[a, p].wait()
                    for k in range(3):
                        tok_s[a, p, k].wait_recv()
        else:
            ready(j - 1)
            hidden(j - 1, 3)
        if j < 2 * PIECES:
            forward_last(j)
    for i in range(nc, 2 * PIECES):
        forward_last(i)
    ready(nc - 1)
    hidden(nc - 1, 3)
    for p in range(PIECES):
        for a in range(2):
            tok_s[a, p, 3].wait_recv()

    grads = ((pv, rxv, rhv, dg), (pu, rxu, rhu, ug))
    cross, over, back = {}, {}, {}

    def send_x(g, j, first):
        part, rx = grads[g][0], grads[g][1]
        half = 1 - h if first else h
        c = links.remote(part.at[j, half, :, 1 - x], rx.at[j, half], dev_x)
        links.start(c)
        cross[g, j, first] = c

    def gradients(j):
        for first in (True, False):
            half = 1 - h if first else h

            def down_block(b):
                span = pl.ds(pl.multiple_of((half * nq + b) * 2 * rows, 2 * rows), 2 * rows)
                term = product(act[j], cs[:, span], 0, 0).astype(bf16)
                pv[j, half, b, 0] = term[:, :rows]
                pv[j, half, b, 1] = term[:, rows:]

            loop(nq, down_block)
            send_x(0, j, first)
        for first in (True, False):
            half = 1 - h if first else h

            def up_block(b):
                span = pl.ds(pl.multiple_of((half * nq + b) * 2 * rows, 2 * rows), 2 * rows)
                term = product(xs[:, span], pre_grad[j], 0, 0).astype(bf16)
                pu[j, half, b] = term.reshape(2, rows, fc)

            loop(nq, up_block)
            send_x(1, j, first)

    def reduce_far(j):
        for g, (part, rx, rh, _) in enumerate(grads):
            cross[g, j, True].wait_recv()

            def add(b):
                total = part[j, 1 - h, b, x].astype(f32) + rx[j, 1 - h, b].astype(f32)
                part[j, 1 - h, b, x] = total.astype(bf16)

            loop(nq, add)
            c = links.remote(part.at[j, 1 - h, :, x], rh.at[j], dev_h)
            links.start(c)
            over[g, j] = c

    def finish(j):
        for g, (part, rx, rh, out) in enumerate(grads):
            cross[g, j, False].wait_recv()
            over[g, j].wait_recv()

            def add(b):
                total = part[j, h, b, x].astype(f32) + rx[j, h, b].astype(f32)
                total = (total + rh[j, b].astype(f32)) * scale
                part[j, h, b, x] = total.astype(bf16)

            loop(nq, add)
            for k, (device, other) in enumerate(hid):
                c = links.remote(part.at[j, h, other, x], out.at[q, j], device)
                links.start(c)
                back[g, j, k] = c
            out[q, j] = part[j, h, q, x]

    order = (qd, qy, ql, q)
    swap = {}

    def input_part(i):
        span = pl.ds(pl.multiple_of(order[i] * tl, tl), tl)
        slot = i % 2
        if i >= 2:
            swap[i - 2].wait_send()

        def columns_of(half, b, put):
            total = product(pre_grad[0, span, :], us[0, half, b].reshape(-1, fc), 1, 1)
            for j in range(1, nc):
                total += product(
                    pre_grad[j, span, :], us[j, half, b].reshape(-1, fc), 1, 1
                )
            put(pl.ds(pl.multiple_of(b * 2 * rows, 2 * rows), 2 * rows), total.astype(bf16))

        def to_sib(cols, value):
            sib_out[slot, :, cols] = value

        def to_own(cols, value):
            own[i, :, cols] = value

        loop(nq, lambda b: columns_of(1 - tp, b, to_sib))
        if i >= 2:
            pl.semaphore_wait(credit, 1)
        swap[i] = links.remote(sib_out.at[slot], sib_in.at[slot], dev_s)
        swap[i].start()
        loop(nq, lambda b: columns_of(tp, b, to_own))

    steps = 4
    step = tl // steps

    def join(i):
        swap[i].wait_recv()

        def add(b):
            span = pl.ds(pl.multiple_of(b * step, step), step)
            total = own[i, span, :].astype(f32) + sib_in[i % 2, span, :].astype(f32)
            own[i, span, :] = total.astype(bf16)

        loop(steps, add)
        if i < 2:
            pl.semaphore_signal(credit, inc=1, device_id=dev_s, device_id_type=MESH)

    hidden(0, 1)
    gradients(0)
    hidden(1, 1)
    gradients(1)
    reduce_far(0)
    for j in range(2, nc):
        hidden(j, 1)
    input_part(0)
    input_part(1)
    gradients(2)
    to_y = []
    for i in range(2):
        join(i)
        to_y.append(links.remote(own.at[i], ry.at[i], dev_y))
        links.start(to_y[i])
    reduce_far(1)
    input_part(2)
    input_part(3)
    for j in range(3, nc):
        gradients(j)
    finish(0)
    reduce_far(2)
    join(2)
    join(3)
    to_y[0].wait_recv()

    def add_y(b):
        span = pl.ds(pl.multiple_of(b * step, step), step)
        total = own[2, span, :].astype(f32) + ry[0, span, :].astype(f32)
        own[2, span, :] = total.astype(bf16)

    loop(steps, add_y)
    to_l = links.remote(own.at[2], rl, dev_l)
    links.start(to_l)
    finish(1)
    for j in range(3, nc):
        reduce_far(j)
    to_y[1].wait_recv()
    to_l.wait_recv()

    def add_last(b):
        span = pl.ds(pl.multiple_of(b * step, step), step)
        total = own[3, span, :].astype(f32) + ry[1, span, :].astype(f32)
        og[span, :] = (total + rl[span, :].astype(f32)).astype(bf16)

    loop(steps, add_last)
    for j in range(2, nc):
        finish(j)
    for c in back.values():
        c.wait_recv()
    swap[2].wait_send()
    swap[3].wait_send()
    for c in links.started:
        c.wait_send()


def pair_device(normed_input, cotangent, up_weight, down_weight):
    tl, wl = normed_input.shape
    rows, fl = up_weight.shape
    tokens, width = tl * lax.axis_size("fs"), wl * lax.axis_size("tp")
    scale = float(tokens) ** -0.5
    fb = fl // 4
    fc = fb // CHUNKS
    nc, nq = CHUNKS, 4
    bf16 = jnp.bfloat16
    many = 160
    near = tokens // 4
    vmem = pl.BlockSpec(memory_space=pltpu.VMEM)
    flops = 10 * near * width * fb
    og, ug, dg = pl.pallas_call(
        functools.partial(pair_kernel, scale),
        out_shape=(
            jax.ShapeDtypeStruct((tl, wl), bf16),
            jax.ShapeDtypeStruct((nq, nc, rows, fc), bf16),
            jax.ShapeDtypeStruct((nq, nc, fc, rows), bf16),
        ),
        in_specs=[pl.BlockSpec(memory_space=pl.ANY)] * 4,
        out_specs=(vmem,) * 3,
        scratch_shapes=[
            pltpu.VMEM((near, width), bf16),
            pltpu.VMEM((near, width), bf16),
            pltpu.VMEM((nc, 2, nq, 2, rows, fc), bf16),
            pltpu.VMEM((nc, 2, nq, 2, fc, rows), bf16),
            pltpu.VMEM((nc, near, fc), bf16),
            pltpu.VMEM((nc, near, fc), bf16),
            pltpu.VMEM((nc, 2, nq, 2, rows, fc), bf16),
            pltpu.VMEM((nc, 2, nq, 2, fc, rows), bf16),
            pltpu.VMEM((nc, 2, nq, rows, fc), bf16),
            pltpu.VMEM((nc, 2, nq, fc, rows), bf16),
            pltpu.VMEM((nc, nq, rows, fc), bf16),
            pltpu.VMEM((nc, nq, fc, rows), bf16),
            pltpu.VMEM((4, tl, wl), bf16),
            pltpu.VMEM((2, tl, wl), bf16),
            pltpu.VMEM((2, tl, wl), bf16),
            pltpu.VMEM((2, tl, wl), bf16),
            pltpu.VMEM((tl, wl), bf16),
            pltpu.SemaphoreType.DMA((many,)),
            pltpu.SemaphoreType.DMA((many,)),
            pltpu.SemaphoreType.DMA((2 * nc + 2 * PIECES,)),
            pltpu.SemaphoreType.REGULAR,
        ],
        compiler_params=pltpu.CompilerParams(
            collective_id=0, has_side_effects=True, vmem_limit_bytes=67043328
        ),
        cost_estimate=pl.CostEstimate(
            flops=flops, bytes_accessed=8 * tl * wl, transcendentals=0
        ),
        name="pairs",
    )(normed_input, cotangent, up_weight, down_weight)
    up_grad = jnp.moveaxis(ug, 2, 0).reshape(rows, fl).astype(jnp.float32)
    down_grad = dg.reshape(fl, rows).astype(jnp.float32)
    return og, up_grad, down_grad


def solution(mesh):
    fs, tp = mesh.shape["fs"], mesh.shape["tp"]
    if fs != 2**4 or tp != 2:
        return collective_solution(mesh)
    in_specs = (P("fs", "tp"), P("fs", "tp"), P("fs", "tp"), P("tp", "fs"))
    out_specs = (P("fs", "tp"), P("fs", "tp"), P("tp", "fs"))
    return jax.shard_map(
        pair_device, mesh=mesh, in_specs=in_specs, out_specs=out_specs, check_vma=False
    )
```

```python
import functools

import jax
import jax.numpy as jnp
from jax import lax
from jax.experimental import pallas as pl
from jax.experimental.pallas import tpu as pltpu
from jax.sharding import Mesh, PartitionSpec as P


def hidden_ways(size):
    return 4 if size % 4 == 0 and size > 4 else 1


def right_product(left, right):
    return lax.dot_general(
        left, right, (((1,), (1,)), ((), ())), preferred_element_type=jnp.float32
    )


def left_product(left, right):
    return lax.dot_general(
        left, right, (((0,), (0,)), ((), ())), preferred_element_type=jnp.float32
    )


def swap(array, k):
    ways = lax.axis_size("hid")
    return lax.ppermute(array, "hid", [(i, i ^ k) for i in range(ways)])


def gather_tokens(array):
    ways = lax.axis_size("hid")
    pieces = [array] + [swap(array, k) for k in range(1, ways)]
    array = jnp.concatenate(pieces, axis=0)
    return lax.all_gather(array, "tp", axis=1, tiled=True)


def scatter_tokens(array):
    ways = lax.axis_size("hid")
    pieces = jnp.split(array, ways, axis=0)
    total = pieces[0].astype(jnp.float32)
    for k in range(1, ways):
        total = total + swap(pieces[k], k).astype(jnp.float32)
    return total.astype(array.dtype)


def exchange(blocks):
    ways, me = lax.axis_size("hid"), lax.axis_index("hid")
    got = []
    for k in range(ways):
        block = lax.dynamic_index_in_dim(blocks, me ^ k, 0, keepdims=False)
        got.append(swap(block, k) if k else block)
    got = jnp.stack(got)
    return [
        lax.dynamic_index_in_dim(got, me ^ j, 0, keepdims=False) for j in range(ways)
    ]


def weight_columns(shard):
    ways = lax.axis_size("hid")
    depth, width = shard.shape
    blocks = jnp.moveaxis(shard.reshape(depth, ways, width // ways), 1, 0)
    return jnp.concatenate(exchange(blocks), axis=0)


def scatter_grad(term):
    ways = lax.axis_size("hid")
    width = term.shape[1]
    term = lax.psum_scatter(term, "tok", scatter_dimension=0, tiled=True)
    return jnp.concatenate(exchange(term.reshape(ways, -1, width)), axis=1)


def per_device(normed_input, cotangent, up_weight, down_weight):
    tokens = normed_input.shape[0] * lax.axis_size("tok") * lax.axis_size("hid")
    scale = lax.rsqrt(jnp.asarray(tokens, jnp.float32))
    up_rows = weight_columns(up_weight)
    down_rows = weight_columns(down_weight.T)
    up_rows, down_rows, normed_input, cotangent = lax.optimization_barrier(
        (up_rows, down_rows, normed_input, cotangent)
    )
    block_up = lax.all_gather(up_rows, "tok", axis=0, tiled=True)
    block_down = lax.all_gather(down_rows, "tok", axis=0, tiled=True)
    whole_input = gather_tokens(normed_input)
    whole_cot = gather_tokens(cotangent)
    pre = jnp.dot(whole_input, block_up, preferred_element_type=jnp.float32)
    rectified = jax.nn.relu(pre)
    act = (rectified * rectified).astype(jnp.bfloat16)
    down_term = left_product(whole_cot, act) * scale
    down_grad = scatter_grad(down_term.astype(jnp.bfloat16)).astype(jnp.float32).T
    act_grad = jnp.dot(whole_cot, block_down, preferred_element_type=jnp.float32)
    pre_grad = (2.0 * rectified * act_grad).astype(jnp.bfloat16)
    up_term = left_product(whole_input, pre_grad) * scale
    up_grad = scatter_grad(up_term.astype(jnp.bfloat16)).astype(jnp.float32)
    partial_value = right_product(pre_grad, block_up).astype(jnp.bfloat16)
    input_grad = lax.psum_scatter(
        partial_value, "tp", scatter_dimension=1, tiled=True
    )
    input_grad = scatter_tokens(input_grad)
    return (input_grad, up_grad, down_grad)


def collective_solution(mesh):
    fs, tp = mesh.shape["fs"], mesh.shape["tp"]
    ways = hidden_ways(fs)
    fine = Mesh(
        mesh.devices.reshape(fs // ways, ways, tp), ("tok", "hid", "tp")
    )
    rows = ("tok", "hid")
    in_specs = (P(rows, "tp"), P(rows, "tp"), P(rows, "tp"), P("tp", rows))
    out_specs = (P(rows, "tp"), P(rows, "tp"), P("tp", rows))
    return jax.shard_map(
        per_device, mesh=fine, in_specs=in_specs, out_specs=out_specs, check_vma=False
    )


MESH = pl.DeviceIdType.MESH
CHUNKS = 4
PIECES = 8


class Links:
    def __init__(self, send, recv, local):
        self.send, self.recv, self.local = send, recv, local
        self.slots, self.groups, self.used_local = {}, {}, 0

    def remote(self, src, dst, device, group, slot):
        send = self.groups.setdefault(group, len(self.groups))
        recv = self.slots.setdefault(slot, len(self.slots))
        return pltpu.make_async_remote_copy(
            src_ref=src,
            dst_ref=dst,
            send_sem=self.send.at[send],
            recv_sem=self.recv.at[recv],
            device_id=device,
            device_id_type=MESH,
        )

    def arrived(self, slot, size_of):
        sem = self.recv.at[self.slots[slot]]
        pltpu.make_async_copy(size_of, size_of, sem).wait()

    def sent(self, group, size_of):
        sem = self.send.at[self.groups[group]]
        pltpu.make_async_copy(size_of, size_of, sem).wait()

    def copy(self, src, dst):
        i = self.used_local
        self.used_local += 1
        copy = pltpu.make_async_copy(src, dst, self.local.at[i])
        copy.start()
        return copy


def loop(n, body):
    def step(i, carry):
        body(i)
        return carry

    lax.fori_loop(0, n, step, 0)


def product(left, right, left_dim, right_dim):
    return lax.dot_general(
        left,
        right,
        (((left_dim,), (right_dim,)), ((), ())),
        preferred_element_type=jnp.float32,
    )


def pair_kernel(
    scale,
    x_hbm,
    c_hbm,
    u_hbm,
    v_hbm,
    og,
    ug,
    dg,
    xs,
    cs,
    us,
    vs,
    act,
    pre_grad,
    pu,
    pv,
    rxu,
    rxv,
    rhu,
    rhv,
    own,
    sib_out,
    sib_in,
    ry,
    rl,
    send,
    recv,
    local,
    credit,
    turn,
):
    bf16, f32 = jnp.bfloat16, jnp.float32
    tl, wl = x_hbm.shape
    nc, _, nq, _, rows, fc = us.shape
    fs, tp = lax.axis_index("fs"), lax.axis_index("tp")
    x, y = fs % 2, (fs // 2) % 2
    l, h = (fs // 4) % 2, fs // 8
    q, qy, ql, qd = l * 2 + y, l * 2 + 1 - y, (1 - l) * 2 + y, (1 - l) * 2 + 1 - y
    dev_x, dev_y = (fs + 1 - 2 * x, tp), (fs + 2 - 4 * y, tp)
    dev_l, dev_h = (fs + 4 - 8 * l, tp), (fs + 8 - 16 * h, tp)
    dev_d, dev_s = (fs + 6 - 4 * y - 8 * l, tp), (fs, 1 - tp)
    hid = ((dev_d, qd), (dev_y, qy), (dev_l, ql))
    links = Links(send, recv, local)
    weights = ((us, u_hbm, 1), (vs, v_hbm, 0))

    barrier = pltpu.get_barrier_semaphore()
    for device in (dev_x, dev_y, dev_l, dev_h, dev_d, dev_s):
        pl.semaphore_signal(barrier, inc=1, device_id=device, device_id_type=MESH)
    pl.semaphore_wait(barrier, 6)

    def columns(hbm, dim, block):
        span = pl.ds(pl.multiple_of(block * fc, fc), fc)
        return hbm.at[:, span] if dim else hbm.at[span, :]

    mine = {}
    for j in range(nc):
        for w, (buf, hbm, dim) in enumerate(weights):
            mine[w, j] = links.copy(columns(hbm, dim, q * nc + j), buf.at[j, h, q, x])
            for device, other in hid:
                src = columns(hbm, dim, other * nc + j)
                dst = buf.at[j, h, q, x]
                links.remote(src, dst, device, "own", ("spread", w, j)).start()

    tr = tl // PIECES
    mine_cols = pl.ds(pl.multiple_of(tp * wl, wl), wl)
    tokens = ((xs, x_hbm), (cs, c_hbm))

    def spot(buf, group, p):
        return buf.at[pl.ds(pl.multiple_of(group * tl + p * tr, tr), tr), mine_cols]

    own_tok = []
    for p in range(PIECES):
        for buf, hbm in tokens:
            src, dst = hbm.at[pl.ds(p * tr, tr), :], spot(buf, q, p)
            own_tok.append(links.copy(src, dst))
            links.remote(src, dst, dev_l, "own", ("l", p)).start()
            links.remote(src, dst, dev_y, "own", "y").start()
            links.remote(src, dst, dev_s, "own", "s0").start()

    far, second, near, pass_l, pass_d, pass_y = {}, {}, {}, {}, {}, []
    for j in range(nc):
        for w, (buf, _, _) in enumerate(weights):
            block = buf.at[j, h, :, x]
            far[w, j] = links.remote(block, block, dev_h, "far", ("far", w, j))
            near[w, j] = links.remote(block, block, dev_x, "x", ("ready", j))
            block = buf.at[j, 1 - h, :, x]
            second[w, j] = links.remote(block, block, dev_x, "x", ("ready", j))
    for p in range(PIECES):
        pass_l[p], pass_d[p] = [], []
        for buf, _ in tokens:
            block = spot(buf, ql, p)
            pass_l[p].append(links.remote(block, block, dev_y, "pass", ("d", p)))
            pass_l[p].append(links.remote(block, block, dev_s, "pass", "s1"))
            block = spot(buf, qy, p)
            pass_y.append(links.remote(block, block, dev_s, "pass", "s2"))
            block = spot(buf, qd, p)
            pass_d[p].append(links.remote(block, block, dev_s, "pass", "s3"))
    piece_pair = xs.at[pl.ds(0, tr)]
    token_pair = xs.at[pl.ds(0, tl)]

    def pass_near(j):
        for w, (buf, _, _) in enumerate(weights):
            mine[w, j].wait()
            links.arrived(("spread", w, j), buf.at[j, h, pl.ds(0, 3), x])
            near[w, j].start()

    def pass_far(j):
        for w in range(2):
            far[w, j].wait_recv()
            second[w, j].start()

    def pass_token(p):
        links.arrived(("l", p), piece_pair)
        for c in pass_l[p]:
            c.start()

    def pass_last(p):
        links.arrived(("d", p), piece_pair)
        for c in pass_d[p]:
            c.start()

    def far_sent():
        links.sent("far", token_pair)

    def hidden(j, low, high):
        down = lambda: jnp.concatenate(
            [vs[j, a, b, c] for a in range(2) for b in range(nq) for c in range(2)],
            axis=1,
        )

        def one(k):
            group = 2 * (l + (k // 2) * (1 - 2 * l)) + y + (k % 2) * (1 - 2 * y)
            span = pl.ds(pl.multiple_of(group * tl, tl), tl)
            pre = product(xs[span, :], us[j].reshape(-1, fc), 1, 0)
            rectified = jnp.maximum(pre, 0.0)
            act[j, span, :] = (rectified * rectified).astype(bf16)
            act_grad = product(cs[span, :], down(), 1, 1)
            pre_grad[j, span, :] = (2.0 * rectified * act_grad).astype(bf16)

        if high == low + 1:
            one(low)
        else:
            loop(high - low, lambda k: one(k + low))

    def ready(j):
        links.arrived(("ready", j), us.at[j])

    outer = 1 - (h + l) % 2
    for j in range(nc):
        pass_near(j)

    @pl.when(outer == 1)
    def _():
        for j in range(nc):
            pass_far(j)
        pl.semaphore_wait(turn, 1)
        for c in far.values():
            c.start()

    @pl.when(outer == 0)
    def _():
        for c in far.values():
            c.start()
        for p in range(PIECES):
            pass_token(p)
        far_sent()
        pl.semaphore_signal(turn, inc=1, device_id=dev_l, device_id_type=MESH)

    links.arrived("y", token_pair)
    for c in pass_y:
        c.start()
    for c in own_tok:
        c.wait()
    links.arrived("s0", token_pair)
    links.arrived("s2", token_pair)

    share = PIECES // nc

    @pl.when(outer == 1)
    def _():
        for j in range(nc):
            for p in range(j * share, (j + 1) * share):
                pass_token(p)
            ready(j)
            hidden(j, 0, 2)
        links.arrived("s1", token_pair)
        for j in range(nc):
            hidden(j, 2, 3)
        for p in range(PIECES):
            pass_last(p)
        far_sent()

    @pl.when(outer == 0)
    def _():
        links.arrived("s1", token_pair)
        for j in range(nc):
            pass_far(j)
            for p in range(j * share, (j + 1) * share):
                pass_last(p)
            if j:
                ready(j - 1)
                hidden(j - 1, 0, 3)
        ready(nc - 1)
        hidden(nc - 1, 0, 3)

    links.arrived("s3", token_pair)

    def down_spot(group, j):
        return dg.at[group, j]

    def up_spot(group, j):
        return ug.at[:, pl.ds(pl.multiple_of((group * nc + j) * fc, fc), fc)]

    grads = ((pv, rxv, rhv, down_spot), (pu, rxu, rhu, up_spot))
    cross, over = {}, {}

    def send_x(g, j, first):
        part, rx = grads[g][0], grads[g][1]
        half = 1 - h if first else h
        src, dst = part.at[j, half, :, 1 - x], rx.at[j, half]
        cross[g, j, first] = links.remote(src, dst, dev_x, "cross", (g, j, first))
        cross[g, j, first].start()

    def gradient(g, j, first):
        half = 1 - h if first else h

        def block(b):
            span = (half * nq + b) * 2 * rows
            span = pl.ds(pl.multiple_of(span, 2 * rows), 2 * rows)
            if g == 0:
                term = product(act[j], cs[:, span], 0, 0).astype(bf16)
                pv[j, half, b, 0] = term[:, :rows]
                pv[j, half, b, 1] = term[:, rows:]
            else:
                term = product(xs[:, span], pre_grad[j], 0, 0).astype(bf16)
                pu[j, half, b] = term.reshape(2, rows, fc)

        loop(nq, block)
        send_x(g, j, first)

    def reduce_far(g, j):
        part, rx, rh, _ = grads[g]
        cross[g, j, True].wait_recv()

        def add(b):
            total = part[j, 1 - h, b, x].astype(f32) + rx[j, 1 - h, b].astype(f32)
            part[j, 1 - h, b, x] = total.astype(bf16)

        loop(nq, add)
        src, dst = part.at[j, 1 - h, :, x], rh.at[j]
        over[g, j] = links.remote(src, dst, dev_h, "last", ("over", g, j))
        over[g, j].start()

    def finish(g, j):
        part, rx, rh, place = grads[g]
        cross[g, j, False].wait_recv()
        over[g, j].wait_recv()

        def add(b):
            total = part[j, h, b, x].astype(f32) + rx[j, h, b].astype(f32)
            total = (total + rh[j, b].astype(f32)) * scale
            part[j, h, b, x] = total.astype(bf16)

        loop(nq, add)
        for device, other in hid:
            src, dst = part.at[j, h, other, x], place(q, j)
            links.remote(src, dst, device, "last", "back").start()
        place(q, j)[...] = part[j, h, q, x]

    order = (qd, qy, ql, q)
    swap = {}

    turns = {0: 0, 2: 1, 1: 2, 3: 3}

    def input_part(i):
        span = pl.ds(pl.multiple_of(order[i] * tl, tl), tl)
        slot = turns[i] % 2
        if turns[i] >= 2:
            swap[slot].wait_send()

        def columns_of(half, b, put):
            total = product(pre_grad[0, span, :], us[0, half, b].reshape(-1, fc), 1, 1)
            for j in range(1, nc):
                total += product(
                    pre_grad[j, span, :], us[j, half, b].reshape(-1, fc), 1, 1
                )
            put(pl.ds(pl.multiple_of(b * 2 * rows, 2 * rows), 2 * rows), total.astype(bf16))

        def to_sib(cols, value):
            sib_out[slot, :, cols] = value

        def to_own(cols, value):
            own[i, :, cols] = value

        loop(nq, lambda b: columns_of(1 - tp, b, to_sib))
        if turns[i] >= 2:
            pl.semaphore_wait(credit, 1)
        src, dst = sib_out.at[slot], sib_in.at[slot]
        swap[turns[i]] = links.remote(src, dst, dev_s, ("swap", slot), ("swap", i))
        swap[turns[i]].start()
        loop(nq, lambda b: columns_of(tp, b, to_own))

    steps = 4
    step = tl // steps

    def join(i):
        swap[turns[i]].wait_recv()

        def add(b):
            span = pl.ds(pl.multiple_of(b * step, step), step)
            total = own[i, span, :].astype(f32) + sib_in[turns[i] % 2, span, :].astype(f32)
            own[i, span, :] = total.astype(bf16)

        loop(steps, add)
        if turns[i] < 2:
            pl.semaphore_signal(credit, inc=1, device_id=dev_s, device_id_type=MESH)

    to_y, to_l = {}, {}

    def rows_of(b):
        return pl.ds(b * step, step)

    def send_y(i):
        for b in range(steps):
            src, dst = own.at[i, rows_of(b)], ry.at[i, rows_of(b)]
            to_y[i, b] = links.remote(src, dst, dev_y, "last", ("sum_y", i, b))
            to_y[i, b].start()

    def pass_sum(b):
        to_y[0, b].wait_recv()
        total = own[2, rows_of(b)].astype(f32) + ry[0, rows_of(b)].astype(f32)
        own[2, rows_of(b)] = total.astype(bf16)
        src, dst = own.at[2, rows_of(b)], rl.at[rows_of(b)]
        to_l[b] = links.remote(src, dst, dev_l, "last", ("sum_l", b))
        to_l[b].start()

    def last_sum(b):
        to_y[1, b].wait_recv()
        to_l[b].wait_recv()
        total = own[3, rows_of(b)].astype(f32) + ry[1, rows_of(b)].astype(f32)
        og[rows_of(b)] = (total + rl[rows_of(b)].astype(f32)).astype(bf16)

    DOWN, UP, FAR, NEAR = 0, 1, True, False
    hidden(0, 3, 4)
    gradient(DOWN, 0, FAR)
    gradient(UP, 0, FAR)
    hidden(1, 3, 4)
    hidden(2, 3, 4)
    hidden(3, 3, 4)
    gradient(DOWN, 0, NEAR)
    reduce_far(DOWN, 0)
    input_part(0)
    join(0)
    send_y(0)
    reduce_far(UP, 0)
    gradient(UP, 0, NEAR)
    gradient(DOWN, 1, FAR)
    gradient(UP, 1, FAR)
    input_part(2)
    join(2)
    pass_sum(0)
    pass_sum(1)
    finish(DOWN, 0)
    gradient(DOWN, 1, NEAR)
    reduce_far(DOWN, 1)
    pass_sum(2)
    gradient(UP, 1, NEAR)
    finish(UP, 0)
    reduce_far(UP, 1)
    pass_sum(3)
    input_part(1)
    gradient(DOWN, 2, FAR)
    gradient(UP, 2, FAR)
    join(1)
    send_y(1)
    input_part(3)
    join(3)
    finish(DOWN, 1)
    gradient(DOWN, 3, FAR)
    finish(UP, 1)
    gradient(UP, 3, FAR)
    reduce_far(DOWN, 2)
    gradient(DOWN, 2, NEAR)
    reduce_far(UP, 2)
    gradient(UP, 2, NEAR)
    gradient(DOWN, 3, NEAR)
    gradient(UP, 3, NEAR)
    reduce_far(DOWN, 3)
    reduce_far(UP, 3)
    finish(DOWN, 2)
    finish(UP, 2)
    for b in range(steps):
        last_sum(b)
    finish(DOWN, 3)
    finish(UP, 3)
    links.arrived("back", xs.at[pl.ds(0, 3 * tl // 4)])
    swap[2].wait_send()
    swap[3].wait_send()
    links.sent("own", xs.at[pl.ds(0, 15 * tl // 4)])
    links.sent("pass", xs)
    links.sent("x", xs.at[pl.ds(0, 2 * tl)])
    links.sent("cross", xs.at[pl.ds(0, 2 * tl)])
    links.sent("last", xs.at[pl.ds(0, 13 * tl // 4)])


def pair_device(normed_input, cotangent, up_weight, down_weight):
    tl, wl = normed_input.shape
    rows, fl = up_weight.shape
    tokens, width = tl * lax.axis_size("fs"), wl * lax.axis_size("tp")
    scale = float(tokens) ** -0.5
    fb = fl // 4
    fc = fb // CHUNKS
    nc, nq = CHUNKS, 4
    bf16 = jnp.bfloat16
    many = 96
    near = tokens // 4
    vmem = pl.BlockSpec(memory_space=pltpu.VMEM)
    flops = 10 * near * width * fb
    og, ug, dg = pl.pallas_call(
        functools.partial(pair_kernel, scale),
        out_shape=(
            jax.ShapeDtypeStruct((tl, wl), bf16),
            jax.ShapeDtypeStruct((rows, fl), bf16),
            jax.ShapeDtypeStruct((nq, nc, fc, rows), bf16),
        ),
        in_specs=[pl.BlockSpec(memory_space=pl.ANY)] * 4,
        out_specs=(vmem,) * 3,
        scratch_shapes=[
            pltpu.VMEM((near, width), bf16),
            pltpu.VMEM((near, width), bf16),
            pltpu.VMEM((nc, 2, nq, 2, rows, fc), bf16),
            pltpu.VMEM((nc, 2, nq, 2, fc, rows), bf16),
            pltpu.VMEM((nc, near, fc), bf16),
            pltpu.VMEM((nc, near, fc), bf16),
            pltpu.VMEM((nc, 2, nq, 2, rows, fc), bf16),
            pltpu.VMEM((nc, 2, nq, 2, fc, rows), bf16),
            pltpu.VMEM((nc, 2, nq, rows, fc), bf16),
            pltpu.VMEM((nc, 2, nq, fc, rows), bf16),
            pltpu.VMEM((nc, nq, rows, fc), bf16),
            pltpu.VMEM((nc, nq, fc, rows), bf16),
            pltpu.VMEM((4, tl, wl), bf16),
            pltpu.VMEM((2, tl, wl), bf16),
            pltpu.VMEM((2, tl, wl), bf16),
            pltpu.VMEM((2, tl, wl), bf16),
            pltpu.VMEM((tl, wl), bf16),
            pltpu.SemaphoreType.DMA((8,)),
            pltpu.SemaphoreType.DMA((many,)),
            pltpu.SemaphoreType.DMA((2 * nc + 2 * PIECES,)),
            pltpu.SemaphoreType.REGULAR,
            pltpu.SemaphoreType.REGULAR,
        ],
        compiler_params=pltpu.CompilerParams(
            collective_id=0, has_side_effects=True, vmem_limit_bytes=67043328
        ),
        cost_estimate=pl.CostEstimate(
            flops=flops, bytes_accessed=8 * tl * wl, transcendentals=0
        ),
        name="pairs",
    )(normed_input, cotangent, up_weight, down_weight)
    up_grad = ug.astype(jnp.float32)
    down_grad = dg.reshape(fl, rows).astype(jnp.float32)
    return og, up_grad, down_grad


def solution(mesh):
    fs, tp = mesh.shape["fs"], mesh.shape["tp"]
    if fs != 2**4 or tp != 2:
        return collective_solution(mesh)
    in_specs = (P("fs", "tp"), P("fs", "tp"), P("fs", "tp"), P("tp", "fs"))
    out_specs = (P("fs", "tp"), P("fs", "tp"), P("tp", "fs"))
    return jax.shard_map(
        pair_device, mesh=mesh, in_specs=in_specs, out_specs=out_specs, check_vma=False
    )
```

```python
import functools

import jax
import jax.numpy as jnp
from jax import lax
from jax.experimental import pallas as pl
from jax.experimental.pallas import tpu as pltpu
from jax.sharding import Mesh, PartitionSpec as P


def hidden_ways(size):
    return 4 if size % 4 == 0 and size > 4 else 1


def right_product(left, right):
    return lax.dot_general(
        left, right, (((1,), (1,)), ((), ())), preferred_element_type=jnp.float32
    )


def left_product(left, right):
    return lax.dot_general(
        left, right, (((0,), (0,)), ((), ())), preferred_element_type=jnp.float32
    )


def swap(array, k):
    ways = lax.axis_size("hid")
    return lax.ppermute(array, "hid", [(i, i ^ k) for i in range(ways)])


def gather_tokens(array):
    ways = lax.axis_size("hid")
    pieces = [array] + [swap(array, k) for k in range(1, ways)]
    array = jnp.concatenate(pieces, axis=0)
    return lax.all_gather(array, "tp", axis=1, tiled=True)


def scatter_tokens(array):
    ways = lax.axis_size("hid")
    pieces = jnp.split(array, ways, axis=0)
    total = pieces[0].astype(jnp.float32)
    for k in range(1, ways):
        total = total + swap(pieces[k], k).astype(jnp.float32)
    return total.astype(array.dtype)


def exchange(blocks):
    ways, me = lax.axis_size("hid"), lax.axis_index("hid")
    got = []
    for k in range(ways):
        block = lax.dynamic_index_in_dim(blocks, me ^ k, 0, keepdims=False)
        got.append(swap(block, k) if k else block)
    got = jnp.stack(got)
    return [
        lax.dynamic_index_in_dim(got, me ^ j, 0, keepdims=False) for j in range(ways)
    ]


def weight_columns(shard):
    ways = lax.axis_size("hid")
    depth, width = shard.shape
    blocks = jnp.moveaxis(shard.reshape(depth, ways, width // ways), 1, 0)
    return jnp.concatenate(exchange(blocks), axis=0)


def scatter_grad(term):
    ways = lax.axis_size("hid")
    width = term.shape[1]
    term = lax.psum_scatter(term, "tok", scatter_dimension=0, tiled=True)
    return jnp.concatenate(exchange(term.reshape(ways, -1, width)), axis=1)


def per_device(normed_input, cotangent, up_weight, down_weight):
    tokens = normed_input.shape[0] * lax.axis_size("tok") * lax.axis_size("hid")
    scale = lax.rsqrt(jnp.asarray(tokens, jnp.float32))
    up_rows = weight_columns(up_weight)
    down_rows = weight_columns(down_weight.T)
    up_rows, down_rows, normed_input, cotangent = lax.optimization_barrier(
        (up_rows, down_rows, normed_input, cotangent)
    )
    block_up = lax.all_gather(up_rows, "tok", axis=0, tiled=True)
    block_down = lax.all_gather(down_rows, "tok", axis=0, tiled=True)
    whole_input = gather_tokens(normed_input)
    whole_cot = gather_tokens(cotangent)
    pre = jnp.dot(whole_input, block_up, preferred_element_type=jnp.float32)
    rectified = jax.nn.relu(pre)
    act = (rectified * rectified).astype(jnp.bfloat16)
    down_term = left_product(whole_cot, act) * scale
    down_grad = scatter_grad(down_term.astype(jnp.bfloat16)).astype(jnp.float32).T
    act_grad = jnp.dot(whole_cot, block_down, preferred_element_type=jnp.float32)
    pre_grad = (2.0 * rectified * act_grad).astype(jnp.bfloat16)
    up_term = left_product(whole_input, pre_grad) * scale
    up_grad = scatter_grad(up_term.astype(jnp.bfloat16)).astype(jnp.float32)
    partial_value = right_product(pre_grad, block_up).astype(jnp.bfloat16)
    input_grad = lax.psum_scatter(
        partial_value, "tp", scatter_dimension=1, tiled=True
    )
    input_grad = scatter_tokens(input_grad)
    return (input_grad, up_grad, down_grad)


def collective_solution(mesh):
    fs, tp = mesh.shape["fs"], mesh.shape["tp"]
    ways = hidden_ways(fs)
    fine = Mesh(
        mesh.devices.reshape(fs // ways, ways, tp), ("tok", "hid", "tp")
    )
    rows = ("tok", "hid")
    in_specs = (P(rows, "tp"), P(rows, "tp"), P(rows, "tp"), P("tp", rows))
    out_specs = (P(rows, "tp"), P(rows, "tp"), P("tp", rows))
    return jax.shard_map(
        per_device, mesh=fine, in_specs=in_specs, out_specs=out_specs, check_vma=False
    )


MESH = pl.DeviceIdType.MESH
CHUNKS = 4
PIECES = 8


class Links:
    def __init__(self, send, recv, local):
        self.send, self.recv, self.local = send, recv, local
        self.slots, self.groups, self.used_local = {}, {}, 0

    def remote(self, src, dst, device, group, slot):
        send = self.groups.setdefault(group, len(self.groups))
        recv = self.slots.setdefault(slot, len(self.slots))
        return pltpu.make_async_remote_copy(
            src_ref=src,
            dst_ref=dst,
            send_sem=self.send.at[send],
            recv_sem=self.recv.at[recv],
            device_id=device,
            device_id_type=MESH,
        )

    def arrived(self, slot, size_of):
        sem = self.recv.at[self.slots[slot]]
        pltpu.make_async_copy(size_of, size_of, sem).wait()

    def sent(self, group, size_of):
        sem = self.send.at[self.groups[group]]
        pltpu.make_async_copy(size_of, size_of, sem).wait()

    def copy(self, src, dst):
        i = self.used_local
        self.used_local += 1
        copy = pltpu.make_async_copy(src, dst, self.local.at[i])
        copy.start()
        return copy


def loop(n, body):
    def step(i, carry):
        body(i)
        return carry

    lax.fori_loop(0, n, step, 0)


def product(left, right, left_dim, right_dim):
    return lax.dot_general(
        left,
        right,
        (((left_dim,), (right_dim,)), ((), ())),
        preferred_element_type=jnp.float32,
    )


def pair_kernel(
    scale,
    x_hbm,
    c_hbm,
    u_hbm,
    v_hbm,
    og,
    ug,
    dg,
    xs,
    cs,
    us,
    vs,
    act,
    pre_grad,
    pu,
    pv,
    rxu,
    rxv,
    rhu,
    rhv,
    own,
    sib_out,
    sib_in,
    ry,
    rl,
    send,
    recv,
    local,
    credit,
    turn,
):
    bf16, f32 = jnp.bfloat16, jnp.float32
    tl, wl = x_hbm.shape
    nc, _, nq, _, rows, fc = us.shape
    fs, tp = lax.axis_index("fs"), lax.axis_index("tp")
    x, y = fs % 2, (fs // 2) % 2
    l, h = (fs // 4) % 2, fs // 8
    q, qy, ql, qd = l * 2 + y, l * 2 + 1 - y, (1 - l) * 2 + y, (1 - l) * 2 + 1 - y
    dev_x, dev_y = (fs + 1 - 2 * x, tp), (fs + 2 - 4 * y, tp)
    dev_l, dev_h = (fs + 4 - 8 * l, tp), (fs + 8 - 16 * h, tp)
    dev_d, dev_s = (fs + 6 - 4 * y - 8 * l, tp), (fs, 1 - tp)
    hid = ((dev_d, qd), (dev_y, qy), (dev_l, ql))
    links = Links(send, recv, local)
    weights = ((us, u_hbm, 1), (vs, v_hbm, 0))

    barrier = pltpu.get_barrier_semaphore()
    for device in (dev_x, dev_y, dev_l, dev_h, dev_d, dev_s):
        pl.semaphore_signal(barrier, inc=1, device_id=device, device_id_type=MESH)
    pl.semaphore_wait(barrier, 6)

    def columns(hbm, dim, block):
        span = pl.ds(pl.multiple_of(block * fc, fc), fc)
        return hbm.at[:, span] if dim else hbm.at[span, :]

    mine = {}
    for j in range(nc):
        for w, (buf, hbm, dim) in enumerate(weights):
            mine[w, j] = links.copy(columns(hbm, dim, q * nc + j), buf.at[j, h, q, x])
            for device, other in hid:
                src = columns(hbm, dim, other * nc + j)
                dst = buf.at[j, h, q, x]
                links.remote(src, dst, device, "own", ("spread", w, j)).start()

    tr = tl // PIECES
    mine_cols = pl.ds(pl.multiple_of(tp * wl, wl), wl)
    tokens = ((xs, x_hbm), (cs, c_hbm))

    def spot(buf, group, p):
        return buf.at[pl.ds(pl.multiple_of(group * tl + p * tr, tr), tr), mine_cols]

    own_tok = []
    for p in range(PIECES):
        for buf, hbm in tokens:
            src, dst = hbm.at[pl.ds(p * tr, tr), :], spot(buf, q, p)
            own_tok.append(links.copy(src, dst))
            links.remote(src, dst, dev_l, "own", ("l", p)).start()
            links.remote(src, dst, dev_y, "own", "y").start()
            links.remote(src, dst, dev_s, "own", "s0").start()

    far, second, near, pass_l, pass_d, pass_y = {}, {}, {}, {}, {}, []
    for j in range(nc):
        for w, (buf, _, _) in enumerate(weights):
            block = buf.at[j, h, :, x]
            far[w, j] = links.remote(block, block, dev_h, "far", ("far", w, j))
            near[w, j] = links.remote(block, block, dev_x, "x", ("ready", j))
            block = buf.at[j, 1 - h, :, x]
            second[w, j] = links.remote(block, block, dev_x, "x", ("ready", j))
    for p in range(PIECES):
        pass_l[p], pass_d[p] = [], []
        for buf, _ in tokens:
            block = spot(buf, ql, p)
            pass_l[p].append(links.remote(block, block, dev_y, "pass", ("d", p)))
            pass_l[p].append(links.remote(block, block, dev_s, "pass", "s1"))
            block = spot(buf, qy, p)
            pass_y.append(links.remote(block, block, dev_s, "pass", "s2"))
            block = spot(buf, qd, p)
            pass_d[p].append(links.remote(block, block, dev_s, "pass", "s3"))
    piece_pair = xs.at[pl.ds(0, tr)]
    token_pair = xs.at[pl.ds(0, tl)]

    def pass_near(j):
        for w, (buf, _, _) in enumerate(weights):
            mine[w, j].wait()
            links.arrived(("spread", w, j), buf.at[j, h, pl.ds(0, 3), x])
            near[w, j].start()

    def pass_far(j):
        for w in range(2):
            far[w, j].wait_recv()
            second[w, j].start()

    def pass_token(p):
        links.arrived(("l", p), piece_pair)
        for c in pass_l[p]:
            c.start()

    def pass_last(p):
        links.arrived(("d", p), piece_pair)
        for c in pass_d[p]:
            c.start()

    def far_sent():
        links.sent("far", token_pair)

    def hidden(j, low, high):
        down = lambda: jnp.concatenate(
            [vs[j, a, b, c] for a in range(2) for b in range(nq) for c in range(2)],
            axis=1,
        )

        def one(k):
            group = 2 * (l + (k // 2) * (1 - 2 * l)) + y + (k % 2) * (1 - 2 * y)
            span = pl.ds(pl.multiple_of(group * tl, tl), tl)
            pre = product(xs[span, :], us[j].reshape(-1, fc), 1, 0)
            rectified = jnp.maximum(pre, 0.0)
            act[j, span, :] = (rectified * rectified).astype(bf16)
            act_grad = product(cs[span, :], down(), 1, 1)
            pre_grad[j, span, :] = (2.0 * rectified * act_grad).astype(bf16)

        if high == low + 1:
            one(low)
        else:
            loop(high - low, lambda k: one(k + low))

    def ready(j):
        links.arrived(("ready", j), us.at[j])

    outer = 1 - (h + l) % 2
    for j in range(nc):
        pass_near(j)

    @pl.when(outer == 1)
    def _():
        for j in range(nc):
            pass_far(j)
        pl.semaphore_wait(turn, 1)
        for c in far.values():
            c.start()

    @pl.when(outer == 0)
    def _():
        for c in far.values():
            c.start()
        for p in range(PIECES):
            pass_token(p)
        far_sent()
        pl.semaphore_signal(turn, inc=1, device_id=dev_l, device_id_type=MESH)

    links.arrived("y", token_pair)
    for c in pass_y:
        c.start()
    for c in own_tok:
        c.wait()
    links.arrived("s0", token_pair)
    links.arrived("s2", token_pair)

    share = PIECES // nc

    @pl.when(outer == 1)
    def _():
        for j in range(nc):
            for p in range(j * share, (j + 1) * share):
                pass_token(p)
            ready(j)
            hidden(j, 0, 2)
        for p in range(3 * PIECES // 4):
            pass_last(p)
        links.arrived("s1", token_pair)
        hidden(0, 2, 3)
        hidden(1, 2, 3)
        for p in range(3 * PIECES // 4, PIECES):
            pass_last(p)
        far_sent()

    @pl.when(outer == 0)
    def _():
        links.arrived("s1", token_pair)
        for j in range(nc):
            pass_far(j)
            for p in range(j * share, (j + 1) * share):
                pass_last(p)
            if j:
                ready(j - 1)
                hidden(j - 1, 0, 3)

    links.arrived("s3", token_pair)

    def down_spot(group, j):
        return dg.at[group, j]

    def up_spot(group, j):
        return ug.at[:, pl.ds(pl.multiple_of((group * nc + j) * fc, fc), fc)]

    grads = ((pv, rxv, rhv, down_spot), (pu, rxu, rhu, up_spot))
    cross, over = {}, {}

    def send_x(g, j, first):
        part, rx = grads[g][0], grads[g][1]
        half = 1 - h if first else h
        src, dst = part.at[j, half, :, 1 - x], rx.at[j, half]
        cross[g, j, first] = links.remote(src, dst, dev_x, "cross", (g, j, first))
        cross[g, j, first].start()

    def gradient(g, j, first):
        half = 1 - h if first else h

        def block(b):
            span = (half * nq + b) * 2 * rows
            span = pl.ds(pl.multiple_of(span, 2 * rows), 2 * rows)
            if g == 0:
                term = product(act[j], cs[:, span], 0, 0).astype(bf16)
                pv[j, half, b, 0] = term[:, :rows]
                pv[j, half, b, 1] = term[:, rows:]
            else:
                term = product(xs[:, span], pre_grad[j], 0, 0).astype(bf16)
                pu[j, half, b] = term.reshape(2, rows, fc)

        loop(nq, block)
        send_x(g, j, first)

    def reduce_far(g, j):
        part, rx, rh, _ = grads[g]
        cross[g, j, True].wait_recv()

        def add(b):
            total = part[j, 1 - h, b, x].astype(f32) + rx[j, 1 - h, b].astype(f32)
            part[j, 1 - h, b, x] = total.astype(bf16)

        loop(nq, add)
        src, dst = part.at[j, 1 - h, :, x], rh.at[j]
        over[g, j] = links.remote(src, dst, dev_h, "last", ("over", g, j))
        over[g, j].start()

    def finish(g, j):
        part, rx, rh, place = grads[g]
        cross[g, j, False].wait_recv()
        over[g, j].wait_recv()

        def add(b):
            total = part[j, h, b, x].astype(f32) + rx[j, h, b].astype(f32)
            total = (total + rh[j, b].astype(f32)) * scale
            part[j, h, b, x] = total.astype(bf16)

        loop(nq, add)
        for device, other in hid:
            src, dst = part.at[j, h, other, x], place(q, j)
            links.remote(src, dst, device, "last", "back").start()
        place(q, j)[...] = part[j, h, q, x]

    def catch_up():
        @pl.when(outer == 1)
        def _():
            for j in range(2, nc):
                hidden(j, 2, 3)

        @pl.when(outer == 0)
        def _():
            ready(nc - 1)
            hidden(nc - 1, 0, 3)

    order = (qd, qy, ql, q)
    swap = {}

    turns = {0: 0, 2: 1, 1: 2, 3: 3}

    def input_part(i):
        span = pl.ds(pl.multiple_of(order[i] * tl, tl), tl)
        slot = turns[i] % 2
        if turns[i] >= 2:
            swap[slot].wait_send()

        def columns_of(half, b, put):
            total = product(pre_grad[0, span, :], us[0, half, b].reshape(-1, fc), 1, 1)
            for j in range(1, nc):
                total += product(
                    pre_grad[j, span, :], us[j, half, b].reshape(-1, fc), 1, 1
                )
            put(pl.ds(pl.multiple_of(b * 2 * rows, 2 * rows), 2 * rows), total.astype(bf16))

        def to_sib(cols, value):
            sib_out[slot, :, cols] = value

        def to_own(cols, value):
            own[i, :, cols] = value

        loop(nq, lambda b: columns_of(1 - tp, b, to_sib))
        if turns[i] >= 2:
            pl.semaphore_wait(credit, 1)
        src, dst = sib_out.at[slot], sib_in.at[slot]
        swap[turns[i]] = links.remote(src, dst, dev_s, ("swap", slot), ("swap", i))
        swap[turns[i]].start()
        loop(nq, lambda b: columns_of(tp, b, to_own))

    steps = 4
    step = tl // steps

    def join(i):
        swap[turns[i]].wait_recv()

        def add(b):
            span = pl.ds(pl.multiple_of(b * step, step), step)
            total = own[i, span, :].astype(f32) + sib_in[turns[i] % 2, span, :].astype(f32)
            own[i, span, :] = total.astype(bf16)

        loop(steps, add)
        if turns[i] < 2:
            pl.semaphore_signal(credit, inc=1, device_id=dev_s, device_id_type=MESH)

    to_y, to_l = {}, {}

    def rows_of(b):
        return pl.ds(b * step, step)

    def send_y(i):
        for b in range(steps):
            src, dst = own.at[i, rows_of(b)], ry.at[i, rows_of(b)]
            to_y[i, b] = links.remote(src, dst, dev_y, "last", ("sum_y", i, b))
            to_y[i, b].start()

    def pass_sum(b):
        to_y[0, b].wait_recv()
        total = own[2, rows_of(b)].astype(f32) + ry[0, rows_of(b)].astype(f32)
        own[2, rows_of(b)] = total.astype(bf16)
        src, dst = own.at[2, rows_of(b)], rl.at[rows_of(b)]
        to_l[b] = links.remote(src, dst, dev_l, "last", ("sum_l", b))
        to_l[b].start()

    def last_sum(b):
        to_y[1, b].wait_recv()
        to_l[b].wait_recv()
        total = own[3, rows_of(b)].astype(f32) + ry[1, rows_of(b)].astype(f32)
        og[rows_of(b)] = (total + rl[rows_of(b)].astype(f32)).astype(bf16)

    DOWN, UP, FAR, NEAR = 0, 1, True, False
    hidden(0, 3, 4)
    gradient(DOWN, 0, FAR)
    gradient(UP, 0, FAR)
    catch_up()
    hidden(1, 3, 4)
    hidden(2, 3, 4)
    reduce_far(DOWN, 0)
    hidden(3, 3, 4)
    gradient(DOWN, 0, NEAR)
    input_part(0)
    join(0)
    send_y(0)
    reduce_far(UP, 0)
    gradient(UP, 0, NEAR)
    gradient(DOWN, 1, FAR)
    gradient(UP, 1, FAR)
    input_part(2)
    join(2)
    pass_sum(0)
    gradient(DOWN, 1, NEAR)
    reduce_far(DOWN, 1)
    pass_sum(1)
    gradient(UP, 1, NEAR)
    finish(DOWN, 0)
    reduce_far(UP, 1)
    pass_sum(2)
    finish(UP, 0)
    pass_sum(3)
    input_part(1)
    gradient(DOWN, 2, FAR)
    gradient(UP, 2, FAR)
    join(1)
    send_y(1)
    input_part(3)
    join(3)
    finish(DOWN, 1)
    gradient(DOWN, 3, FAR)
    reduce_far(DOWN, 2)
    gradient(UP, 3, FAR)
    gradient(DOWN, 2, NEAR)
    reduce_far(UP, 2)
    gradient(UP, 2, NEAR)
    finish(UP, 1)
    gradient(DOWN, 3, NEAR)
    gradient(UP, 3, NEAR)
    reduce_far(DOWN, 3)
    reduce_far(UP, 3)
    finish(DOWN, 2)
    finish(UP, 2)
    for b in range(steps):
        last_sum(b)
    finish(DOWN, 3)
    finish(UP, 3)
    links.arrived("back", xs.at[pl.ds(0, 3 * tl // 4)])
    swap[2].wait_send()
    swap[3].wait_send()
    links.sent("own", xs.at[pl.ds(0, 15 * tl // 4)])
    links.sent("pass", xs)
    links.sent("x", xs.at[pl.ds(0, 2 * tl)])
    links.sent("cross", xs.at[pl.ds(0, 2 * tl)])
    links.sent("last", xs.at[pl.ds(0, 13 * tl // 4)])


def pair_device(normed_input, cotangent, up_weight, down_weight):
    tl, wl = normed_input.shape
    rows, fl = up_weight.shape
    tokens, width = tl * lax.axis_size("fs"), wl * lax.axis_size("tp")
    scale = float(tokens) ** -0.5
    fb = fl // 4
    fc = fb // CHUNKS
    nc, nq = CHUNKS, 4
    bf16 = jnp.bfloat16
    many = 96
    near = tokens // 4
    vmem = pl.BlockSpec(memory_space=pltpu.VMEM)
    flops = 10 * near * width * fb
    og, ug, dg = pl.pallas_call(
        functools.partial(pair_kernel, scale),
        out_shape=(
            jax.ShapeDtypeStruct((tl, wl), bf16),
            jax.ShapeDtypeStruct((rows, fl), bf16),
            jax.ShapeDtypeStruct((nq, nc, fc, rows), bf16),
        ),
        in_specs=[pl.BlockSpec(memory_space=pl.ANY)] * 4,
        out_specs=(vmem,) * 3,
        scratch_shapes=[
            pltpu.VMEM((near, width), bf16),
            pltpu.VMEM((near, width), bf16),
            pltpu.VMEM((nc, 2, nq, 2, rows, fc), bf16),
            pltpu.VMEM((nc, 2, nq, 2, fc, rows), bf16),
            pltpu.VMEM((nc, near, fc), bf16),
            pltpu.VMEM((nc, near, fc), bf16),
            pltpu.VMEM((nc, 2, nq, 2, rows, fc), bf16),
            pltpu.VMEM((nc, 2, nq, 2, fc, rows), bf16),
            pltpu.VMEM((nc, 2, nq, rows, fc), bf16),
            pltpu.VMEM((nc, 2, nq, fc, rows), bf16),
            pltpu.VMEM((nc, nq, rows, fc), bf16),
            pltpu.VMEM((nc, nq, fc, rows), bf16),
            pltpu.VMEM((4, tl, wl), bf16),
            pltpu.VMEM((2, tl, wl), bf16),
            pltpu.VMEM((2, tl, wl), bf16),
            pltpu.VMEM((2, tl, wl), bf16),
            pltpu.VMEM((tl, wl), bf16),
            pltpu.SemaphoreType.DMA((8,)),
            pltpu.SemaphoreType.DMA((many,)),
            pltpu.SemaphoreType.DMA((2 * nc + 2 * PIECES,)),
            pltpu.SemaphoreType.REGULAR,
            pltpu.SemaphoreType.REGULAR,
        ],
        compiler_params=pltpu.CompilerParams(
            collective_id=0, has_side_effects=True, vmem_limit_bytes=67043328
        ),
        cost_estimate=pl.CostEstimate(
            flops=flops, bytes_accessed=8 * tl * wl, transcendentals=0
        ),
        name="pairs",
    )(normed_input, cotangent, up_weight, down_weight)
    up_grad = ug.astype(jnp.float32)
    down_grad = dg.reshape(fl, rows).astype(jnp.float32)
    return og, up_grad, down_grad


def solution(mesh):
    fs, tp = mesh.shape["fs"], mesh.shape["tp"]
    if fs != 2**4 or tp != 2:
        return collective_solution(mesh)
    in_specs = (P("fs", "tp"), P("fs", "tp"), P("fs", "tp"), P("tp", "fs"))
    out_specs = (P("fs", "tp"), P("fs", "tp"), P("tp", "fs"))
    return jax.shard_map(
        pair_device, mesh=mesh, in_specs=in_specs, out_specs=out_specs, check_vma=False
    )
```

```python
import functools

import jax
import jax.numpy as jnp
from jax import lax
from jax.experimental import pallas as pl
from jax.experimental.pallas import tpu as pltpu
from jax.sharding import Mesh, PartitionSpec as P


def hidden_ways(size):
    return 4 if size % 4 == 0 and size > 4 else 1


def right_product(left, right):
    return lax.dot_general(
        left, right, (((1,), (1,)), ((), ())), preferred_element_type=jnp.float32
    )


def left_product(left, right):
    return lax.dot_general(
        left, right, (((0,), (0,)), ((), ())), preferred_element_type=jnp.float32
    )


def swap(array, k):
    ways = lax.axis_size("hid")
    return lax.ppermute(array, "hid", [(i, i ^ k) for i in range(ways)])


def gather_tokens(array):
    ways = lax.axis_size("hid")
    pieces = [array] + [swap(array, k) for k in range(1, ways)]
    array = jnp.concatenate(pieces, axis=0)
    return lax.all_gather(array, "tp", axis=1, tiled=True)


def scatter_tokens(array):
    ways = lax.axis_size("hid")
    pieces = jnp.split(array, ways, axis=0)
    total = pieces[0].astype(jnp.float32)
    for k in range(1, ways):
        total = total + swap(pieces[k], k).astype(jnp.float32)
    return total.astype(array.dtype)


def exchange(blocks):
    ways, me = lax.axis_size("hid"), lax.axis_index("hid")
    got = []
    for k in range(ways):
        block = lax.dynamic_index_in_dim(blocks, me ^ k, 0, keepdims=False)
        got.append(swap(block, k) if k else block)
    got = jnp.stack(got)
    return [
        lax.dynamic_index_in_dim(got, me ^ j, 0, keepdims=False) for j in range(ways)
    ]


def weight_columns(shard):
    ways = lax.axis_size("hid")
    depth, width = shard.shape
    blocks = jnp.moveaxis(shard.reshape(depth, ways, width // ways), 1, 0)
    return jnp.concatenate(exchange(blocks), axis=0)


def scatter_grad(term):
    ways = lax.axis_size("hid")
    width = term.shape[1]
    term = lax.psum_scatter(term, "tok", scatter_dimension=0, tiled=True)
    return jnp.concatenate(exchange(term.reshape(ways, -1, width)), axis=1)


def per_device(normed_input, cotangent, up_weight, down_weight):
    tokens = normed_input.shape[0] * lax.axis_size("tok") * lax.axis_size("hid")
    scale = lax.rsqrt(jnp.asarray(tokens, jnp.float32))
    up_rows = weight_columns(up_weight)
    down_rows = weight_columns(down_weight.T)
    up_rows, down_rows, normed_input, cotangent = lax.optimization_barrier(
        (up_rows, down_rows, normed_input, cotangent)
    )
    block_up = lax.all_gather(up_rows, "tok", axis=0, tiled=True)
    block_down = lax.all_gather(down_rows, "tok", axis=0, tiled=True)
    whole_input = gather_tokens(normed_input)
    whole_cot = gather_tokens(cotangent)
    pre = jnp.dot(whole_input, block_up, preferred_element_type=jnp.float32)
    rectified = jax.nn.relu(pre)
    act = (rectified * rectified).astype(jnp.bfloat16)
    down_term = left_product(whole_cot, act) * scale
    down_grad = scatter_grad(down_term.astype(jnp.bfloat16)).astype(jnp.float32).T
    act_grad = jnp.dot(whole_cot, block_down, preferred_element_type=jnp.float32)
    pre_grad = (2.0 * rectified * act_grad).astype(jnp.bfloat16)
    up_term = left_product(whole_input, pre_grad) * scale
    up_grad = scatter_grad(up_term.astype(jnp.bfloat16)).astype(jnp.float32)
    partial_value = right_product(pre_grad, block_up).astype(jnp.bfloat16)
    input_grad = lax.psum_scatter(
        partial_value, "tp", scatter_dimension=1, tiled=True
    )
    input_grad = scatter_tokens(input_grad)
    return (input_grad, up_grad, down_grad)


def collective_solution(mesh):
    fs, tp = mesh.shape["fs"], mesh.shape["tp"]
    ways = hidden_ways(fs)
    fine = Mesh(
        mesh.devices.reshape(fs // ways, ways, tp), ("tok", "hid", "tp")
    )
    rows = ("tok", "hid")
    in_specs = (P(rows, "tp"), P(rows, "tp"), P(rows, "tp"), P("tp", rows))
    out_specs = (P(rows, "tp"), P(rows, "tp"), P("tp", rows))
    return jax.shard_map(
        per_device, mesh=fine, in_specs=in_specs, out_specs=out_specs, check_vma=False
    )


MESH = pl.DeviceIdType.MESH
CHUNKS = 4
PIECES = 16


class Links:
    def __init__(self, send, recv, local):
        self.send, self.recv, self.local = send, recv, local
        self.slots, self.groups, self.used_local = {}, {}, 0

    def remote(self, src, dst, device, group, slot):
        send = self.groups.setdefault(group, len(self.groups))
        recv = self.slots.setdefault(slot, len(self.slots))
        return pltpu.make_async_remote_copy(
            src_ref=src,
            dst_ref=dst,
            send_sem=self.send.at[send],
            recv_sem=self.recv.at[recv],
            device_id=device,
            device_id_type=MESH,
        )

    def arrived(self, slot, size_of):
        sem = self.recv.at[self.slots[slot]]
        pltpu.make_async_copy(size_of, size_of, sem).wait()

    def sent(self, group, size_of):
        sem = self.send.at[self.groups[group]]
        pltpu.make_async_copy(size_of, size_of, sem).wait()

    def copy(self, src, dst):
        i = self.used_local
        self.used_local += 1
        copy = pltpu.make_async_copy(src, dst, self.local.at[i])
        copy.start()
        return copy


def loop(n, body):
    def step(i, carry):
        body(i)
        return carry

    lax.fori_loop(0, n, step, 0)


def product(left, right, left_dim, right_dim):
    return lax.dot_general(
        left,
        right,
        (((left_dim,), (right_dim,)), ((), ())),
        preferred_element_type=jnp.float32,
    )


def pair_kernel(
    scale,
    x_hbm,
    c_hbm,
    u_hbm,
    v_hbm,
    og,
    ug,
    dg,
    xs,
    cs,
    us,
    vs,
    act,
    pre_grad,
    pu,
    pv,
    rxu,
    rxv,
    rhu,
    rhv,
    own,
    sib_out,
    sib_in,
    ry,
    rl,
    send,
    recv,
    local,
    credit,
    turn,
):
    bf16, f32 = jnp.bfloat16, jnp.float32
    tl, wl = x_hbm.shape
    nc, _, nq, _, rows, fc = us.shape
    fs, tp = lax.axis_index("fs"), lax.axis_index("tp")
    x, y = fs % 2, (fs // 2) % 2
    l, h = (fs // 4) % 2, fs // 8
    q, qy, ql, qd = l * 2 + y, l * 2 + 1 - y, (1 - l) * 2 + y, (1 - l) * 2 + 1 - y
    dev_x, dev_y = (fs + 1 - 2 * x, tp), (fs + 2 - 4 * y, tp)
    dev_l, dev_h = (fs + 4 - 8 * l, tp), (fs + 8 - 16 * h, tp)
    dev_d, dev_s = (fs + 6 - 4 * y - 8 * l, tp), (fs, 1 - tp)
    hid = ((dev_d, qd), (dev_y, qy), (dev_l, ql))
    links = Links(send, recv, local)
    weights = ((us, u_hbm, 1), (vs, v_hbm, 0))
    block_size, shard_size = rows * fc, tl * wl

    def as_large_as(size):
        return xs.at[pl.ds(0, size // xs.shape[1])]


    barrier = pltpu.get_barrier_semaphore()
    for device in (dev_x, dev_y, dev_l, dev_h, dev_d, dev_s):
        pl.semaphore_signal(barrier, inc=1, device_id=device, device_id_type=MESH)
    pl.semaphore_wait(barrier, 6)

    def columns(hbm, dim, block):
        span = pl.ds(pl.multiple_of(block * fc, fc), fc)
        return hbm.at[:, span] if dim else hbm.at[span, :]

    mine = {}
    for j in range(nc):
        for w, (buf, hbm, dim) in enumerate(weights):
            mine[w, j] = links.copy(columns(hbm, dim, q * nc + j), buf.at[j, h, q, x])
            for device, other in hid:
                src = columns(hbm, dim, other * nc + j)
                dst = buf.at[j, h, q, x]
                links.remote(src, dst, device, "own", ("spread", w, j)).start()

    tr = tl // PIECES
    mine_cols = pl.ds(pl.multiple_of(tp * wl, wl), wl)
    tokens = ((xs, x_hbm), (cs, c_hbm))

    def spot(buf, group, p):
        return buf.at[pl.ds(pl.multiple_of(group * tl + p * tr, tr), tr), mine_cols]

    own_tok = []
    for p in range(PIECES):
        for buf, hbm in tokens:
            src, dst = hbm.at[pl.ds(p * tr, tr), :], spot(buf, q, p)
            own_tok.append(links.copy(src, dst))
            links.remote(src, dst, dev_l, "own", ("l", p)).start()
            links.remote(src, dst, dev_y, "own", "y").start()
            links.remote(src, dst, dev_s, "own", "s0").start()

    far, second, near, pass_l, pass_d, pass_y = {}, {}, {}, {}, {}, []
    for j in range(nc):
        for w, (buf, _, _) in enumerate(weights):
            block = buf.at[j, h, :, x]
            far[w, j] = links.remote(block, block, dev_h, "far", ("far", w, j))
            near[w, j] = links.remote(block, block, dev_x, "x", ("ready", j))
            block = buf.at[j, 1 - h, :, x]
            second[w, j] = links.remote(block, block, dev_x, "x", ("ready", j))
    for p in range(PIECES):
        pass_l[p], pass_d[p] = [], []
        for buf, _ in tokens:
            block = spot(buf, ql, p)
            pass_l[p].append(links.remote(block, block, dev_y, "pass", ("d", p)))
            pass_l[p].append(links.remote(block, block, dev_s, "pass", "s1"))
            block = spot(buf, qy, p)
            pass_y.append(links.remote(block, block, dev_s, "pass", "s2"))
            block = spot(buf, qd, p)
            pass_d[p].append(links.remote(block, block, dev_s, "pass", "s3"))
    piece_pair = xs.at[pl.ds(0, tr)]
    token_pair = xs.at[pl.ds(0, tl)]

    def pass_near(j):
        for w, (buf, _, _) in enumerate(weights):
            mine[w, j].wait()
            links.arrived(("spread", w, j), buf.at[j, h, pl.ds(0, 3), x])
            near[w, j].start()

    def pass_far(j):
        for w in range(2):
            far[w, j].wait_recv()
            second[w, j].start()

    def pass_token(p):
        links.arrived(("l", p), piece_pair)
        for c in pass_l[p]:
            c.start()

    def pass_last(p):
        links.arrived(("d", p), piece_pair)
        for c in pass_d[p]:
            c.start()

    def far_sent():
        links.sent("far", as_large_as(8 * nc * block_size))

    def hidden(j, low, high):
        down = lambda: jnp.concatenate(
            [vs[j, a, b, c] for a in range(2) for b in range(nq) for c in range(2)],
            axis=1,
        )

        def one(k):
            group = 2 * (l + (k // 2) * (1 - 2 * l)) + y + (k % 2) * (1 - 2 * y)
            span = pl.ds(pl.multiple_of(group * tl, tl), tl)
            pre = product(xs[span, :], us[j].reshape(-1, fc), 1, 0)
            rectified = jnp.maximum(pre, 0.0)
            act[j, span, :] = (rectified * rectified).astype(bf16)
            act_grad = product(cs[span, :], down(), 1, 1)
            pre_grad[j, span, :] = (2.0 * rectified * act_grad).astype(bf16)

        if high == low + 1:
            one(low)
        else:
            loop(high - low, lambda k: one(k + low))

    def ready(j):
        links.arrived(("ready", j), us.at[j])

    outer = 1 - (h + l) % 2

    @pl.when(outer == 1)
    def _():
        pass_near(0)
        for j in range(nc - 1):
            pass_far(j)
        for j in range(1, nc):
            pass_near(j)
            if j == 1:
                pl.semaphore_wait(turn, 1)
                for w in range(2):
                    far[w, 0].start()
            for w in range(2):
                far[w, j].start()
        pass_far(nc - 1)

    @pl.when(outer == 0)
    def _():
        for j in range(nc):
            pass_near(j)
            for w in range(2):
                far[w, j].start()
        for p in range(PIECES):
            pass_token(p)
            if p == 5 * PIECES // 8:
                far_sent()
                pl.semaphore_signal(
                    turn, inc=1, device_id=dev_l, device_id_type=MESH
                )

    links.arrived("y", token_pair)
    for c in pass_y:
        c.start()
    for c in own_tok:
        c.wait()
    links.arrived("s0", token_pair)
    links.arrived("s2", token_pair)

    share = PIECES // nc

    @pl.when(outer == 1)
    def _():
        for j in range(nc):
            for p in range(j * share, (j + 1) * share):
                pass_token(p)
            ready(j)
            hidden(j, 0, 2)
        for p in range(3 * PIECES // 4):
            pass_last(p)
        links.arrived("s1", token_pair)
        hidden(0, 2, 3)
        hidden(1, 2, 3)
        for p in range(3 * PIECES // 4, PIECES):
            pass_last(p)
        far_sent()

    @pl.when(outer == 0)
    def _():
        links.arrived("s1", token_pair)
        for j in range(nc):
            pass_far(j)
            for p in range(j * share, (j + 1) * share):
                pass_last(p)
            if j:
                ready(j - 1)
                hidden(j - 1, 0, 3)

    links.arrived("s3", token_pair)

    def down_spot(group, j):
        return dg.at[group, j]

    def up_spot(group, j):
        return ug.at[:, pl.ds(pl.multiple_of((group * nc + j) * fc, fc), fc)]

    grads = ((pv, rxv, rhv, down_spot), (pu, rxu, rhu, up_spot))
    cross, over = {}, {}

    pairs = (2 * (1 - l), 2 * l)

    def gradient(g, j, first):
        half = 1 - h if first else h

        def block(b):
            span = (half * nq + b) * 2 * rows
            span = pl.ds(pl.multiple_of(span, 2 * rows), 2 * rows)
            if g == 0:
                term = product(act[j], cs[:, span], 0, 0).astype(bf16)
                pv[j, half, b, 0] = term[:, :rows]
                pv[j, half, b, 1] = term[:, rows:]
            else:
                term = product(xs[:, span], pre_grad[j], 0, 0).astype(bf16)
                pu[j, half, b] = term.reshape(2, rows, fc)

        part, rx = grads[g][0], grads[g][1]
        for k, (base, size) in enumerate(
            [(base, 2) for base in pairs] if first else [(0, nq)]
        ):
            loop(size, lambda b: block(base + b))
            src = part.at[j, half, pl.ds(base, size), 1 - x]
            dst = rx.at[j, half, pl.ds(base, size)]
            c = links.remote(src, dst, dev_x, "cross", (g, j, first, k))
            c.start()
            cross[g, j, first, k] = c

    def reduce_far(g, j):
        part, rx, rh, _ = grads[g]
        for k, base in enumerate(pairs):
            cross[g, j, True, k].wait_recv()
            for b in (base, base + 1):
                total = part[j, 1 - h, b, x].astype(f32) + rx[j, 1 - h, b].astype(f32)
                part[j, 1 - h, b, x] = total.astype(bf16)
            src = part.at[j, 1 - h, pl.ds(base, 2), x]
            dst = rh.at[j, pl.ds(base, 2)]
            over[g, j, k] = links.remote(src, dst, dev_h, "last", ("over", g, j, k))
            over[g, j, k].start()

    def finish(g, j):
        part, rx, rh, place = grads[g]
        cross[g, j, False, 0].wait_recv()
        for k, base in enumerate(pairs):
            over[g, j, k].wait_recv()
            for b in (base, base + 1):
                total = part[j, h, b, x].astype(f32) + rx[j, h, b].astype(f32)
                total = (total + rh[j, b].astype(f32)) * scale
                part[j, h, b, x] = total.astype(bf16)
            for device, other in ((dev_d, qd), (dev_l, ql)) if k == 0 else ((dev_y, qy),):
                src, dst = part.at[j, h, other, x], place(q, j)
                links.remote(src, dst, device, "last", "back").start()
        place(q, j)[...] = part[j, h, q, x]

    def catch_up():
        @pl.when(outer == 1)
        def _():
            for j in range(2, nc):
                hidden(j, 2, 3)

        @pl.when(outer == 0)
        def _():
            ready(nc - 1)
            hidden(nc - 1, 0, 3)

    order = (qd, qy, ql, q)
    swap = {}

    turns = {0: 0, 2: 1, 1: 2, 3: 3}

    def input_part(i):
        span = pl.ds(pl.multiple_of(order[i] * tl, tl), tl)
        slot = turns[i] % 2
        if turns[i] >= 2:
            swap[slot].wait_send()

        def columns_of(half, b, put):
            total = product(pre_grad[0, span, :], us[0, half, b].reshape(-1, fc), 1, 1)
            for j in range(1, nc):
                total += product(
                    pre_grad[j, span, :], us[j, half, b].reshape(-1, fc), 1, 1
                )
            put(pl.ds(pl.multiple_of(b * 2 * rows, 2 * rows), 2 * rows), total.astype(bf16))

        def to_sib(cols, value):
            sib_out[slot, :, cols] = value

        def to_own(cols, value):
            own[i, :, cols] = value

        loop(nq, lambda b: columns_of(1 - tp, b, to_sib))
        if turns[i] >= 2:
            pl.semaphore_wait(credit, 1)
        src, dst = sib_out.at[slot], sib_in.at[slot]
        swap[turns[i]] = links.remote(src, dst, dev_s, ("swap", slot), ("swap", i))
        swap[turns[i]].start()
        loop(nq, lambda b: columns_of(tp, b, to_own))

    steps = 4
    step = tl // steps

    def join(i):
        swap[turns[i]].wait_recv()

        def add(b):
            span = pl.ds(pl.multiple_of(b * step, step), step)
            total = own[i, span, :].astype(f32) + sib_in[turns[i] % 2, span, :].astype(f32)
            own[i, span, :] = total.astype(bf16)

        loop(steps, add)
        if turns[i] < 2:
            pl.semaphore_signal(credit, inc=1, device_id=dev_s, device_id_type=MESH)

    to_y, to_l = {}, {}

    def rows_of(b):
        return pl.ds(b * step, step)

    def send_y(i):
        for b in range(steps):
            src, dst = own.at[i, rows_of(b)], ry.at[i, rows_of(b)]
            to_y[i, b] = links.remote(src, dst, dev_y, "last", ("sum_y", i, b))
            to_y[i, b].start()

    def pass_sum(b):
        to_y[0, b].wait_recv()
        total = own[2, rows_of(b)].astype(f32) + ry[0, rows_of(b)].astype(f32)
        own[2, rows_of(b)] = total.astype(bf16)
        src, dst = own.at[2, rows_of(b)], rl.at[rows_of(b)]
        to_l[b] = links.remote(src, dst, dev_l, "last", ("sum_l", b))
        to_l[b].start()

    def last_sum(b):
        to_y[1, b].wait_recv()
        to_l[b].wait_recv()
        total = own[3, rows_of(b)].astype(f32) + ry[1, rows_of(b)].astype(f32)
        og[rows_of(b)] = (total + rl[rows_of(b)].astype(f32)).astype(bf16)

    DOWN, UP, FAR, NEAR = 0, 1, True, False
    hidden(0, 3, 4)
    gradient(DOWN, 0, FAR)
    gradient(UP, 0, FAR)
    catch_up()
    hidden(1, 3, 4)
    hidden(2, 3, 4)
    reduce_far(DOWN, 0)
    hidden(3, 3, 4)
    gradient(DOWN, 0, NEAR)
    input_part(0)
    join(0)
    send_y(0)
    reduce_far(UP, 0)
    gradient(UP, 0, NEAR)
    input_part(2)
    finish(DOWN, 0)
    join(2)
    gradient(DOWN, 1, FAR)
    pass_sum(0)
    gradient(UP, 1, FAR)
    gradient(DOWN, 1, NEAR)
    pass_sum(1)
    reduce_far(DOWN, 1)
    gradient(UP, 1, NEAR)
    finish(UP, 0)
    reduce_far(UP, 1)
    pass_sum(2)
    gradient(DOWN, 2, FAR)
    pass_sum(3)
    input_part(1)
    gradient(UP, 2, FAR)
    join(1)
    send_y(1)
    input_part(3)
    join(3)
    finish(DOWN, 1)
    gradient(DOWN, 3, FAR)
    reduce_far(DOWN, 2)
    gradient(UP, 3, FAR)
    gradient(DOWN, 2, NEAR)
    reduce_far(UP, 2)
    gradient(UP, 2, NEAR)
    finish(UP, 1)
    gradient(DOWN, 3, NEAR)
    gradient(UP, 3, NEAR)
    reduce_far(DOWN, 3)
    reduce_far(UP, 3)
    finish(DOWN, 2)
    finish(UP, 2)
    for b in range(steps):
        last_sum(b)
    finish(DOWN, 3)
    finish(UP, 3)
    links.arrived("back", as_large_as(6 * nc * block_size))
    swap[2].wait_send()
    swap[3].wait_send()
    links.sent("own", as_large_as(6 * nc * block_size + 6 * shard_size))
    links.sent("pass", as_large_as(8 * shard_size))
    links.sent("x", as_large_as(16 * nc * block_size))
    links.sent("cross", as_large_as(16 * nc * block_size))
    links.sent("last", as_large_as(14 * nc * block_size + 3 * shard_size))


def pair_device(normed_input, cotangent, up_weight, down_weight):
    tl, wl = normed_input.shape
    rows, fl = up_weight.shape
    tokens, width = tl * lax.axis_size("fs"), wl * lax.axis_size("tp")
    scale = float(tokens) ** -0.5
    fb = fl // 4
    fc = fb // CHUNKS
    nc, nq = CHUNKS, 4
    bf16 = jnp.bfloat16
    many = 128
    near = tokens // 4
    vmem = pl.BlockSpec(memory_space=pltpu.VMEM)
    flops = 10 * near * width * fb
    og, ug, dg = pl.pallas_call(
        functools.partial(pair_kernel, scale),
        out_shape=(
            jax.ShapeDtypeStruct((tl, wl), bf16),
            jax.ShapeDtypeStruct((rows, fl), bf16),
            jax.ShapeDtypeStruct((nq, nc, fc, rows), bf16),
        ),
        in_specs=[pl.BlockSpec(memory_space=pl.ANY)] * 4,
        out_specs=(vmem,) * 3,
        scratch_shapes=[
            pltpu.VMEM((near, width), bf16),
            pltpu.VMEM((near, width), bf16),
            pltpu.VMEM((nc, 2, nq, 2, rows, fc), bf16),
            pltpu.VMEM((nc, 2, nq, 2, fc, rows), bf16),
            pltpu.VMEM((nc, near, fc), bf16),
            pltpu.VMEM((nc, near, fc), bf16),
            pltpu.VMEM((nc, 2, nq, 2, rows, fc), bf16),
            pltpu.VMEM((nc, 2, nq, 2, fc, rows), bf16),
            pltpu.VMEM((nc, 2, nq, rows, fc), bf16),
            pltpu.VMEM((nc, 2, nq, fc, rows), bf16),
            pltpu.VMEM((nc, nq, rows, fc), bf16),
            pltpu.VMEM((nc, nq, fc, rows), bf16),
            pltpu.VMEM((4, tl, wl), bf16),
            pltpu.VMEM((2, tl, wl), bf16),
            pltpu.VMEM((2, tl, wl), bf16),
            pltpu.VMEM((2, tl, wl), bf16),
            pltpu.VMEM((tl, wl), bf16),
            pltpu.SemaphoreType.DMA((8,)),
            pltpu.SemaphoreType.DMA((many,)),
            pltpu.SemaphoreType.DMA((2 * nc + 2 * PIECES,)),
            pltpu.SemaphoreType.REGULAR,
            pltpu.SemaphoreType.REGULAR,
        ],
        compiler_params=pltpu.CompilerParams(
            collective_id=0, has_side_effects=True, vmem_limit_bytes=67043328
        ),
        cost_estimate=pl.CostEstimate(
            flops=flops, bytes_accessed=8 * tl * wl, transcendentals=0
        ),
        name="pairs",
    )(normed_input, cotangent, up_weight, down_weight)
    up_grad = ug.astype(jnp.float32)
    down_grad = dg.reshape(fl, rows).astype(jnp.float32)
    return og, up_grad, down_grad


def solution(mesh):
    fs, tp = mesh.shape["fs"], mesh.shape["tp"]
    if fs != 2**4 or tp != 2:
        return collective_solution(mesh)
    in_specs = (P("fs", "tp"), P("fs", "tp"), P("fs", "tp"), P("tp", "fs"))
    out_specs = (P("fs", "tp"), P("fs", "tp"), P("tp", "fs"))
    return jax.shard_map(
        pair_device, mesh=mesh, in_specs=in_specs, out_specs=out_specs, check_vma=False
    )
```
